32 devices in a mesh: ra: 8 (over z, y), cb: 4 (over x, core).
Axes of the slice: x: 2, y: 2, z: 4, core: 2. Of those that a mesh axis runs over, the one named last changes fastest.
Arguments:
- tokens: bfloat16 [512, 4096], P(None, 'ra'), may hold values from -4 to 4, as said below
- pre_gain_first: float32 [4096], P('ra'), may hold values from 0.1 to 1.9
- gate_first: bfloat16 [4096, 11264], P('ra', 'cb'), may hold values from -0.125 to 0.125
- up_first: bfloat16 [4096, 11264], P('ra', 'cb'), may hold values from -0.125 to 0.125
- down_first: bfloat16 [11264, 4096], P('cb', 'ra'), may hold values from -0.078125 to 0.078125
- post_gain_first: float32 [4096], P('ra'), may hold values from 0.1 to 1.9
- pre_gain_second: float32 [4096], P('ra'), may hold values from 0.1 to 1.9
- gate_second: bfloat16 [4096, 11264], P('ra', 'cb'), may hold values from -0.125 to 0.125
- up_second: bfloat16 [4096, 11264], P('ra', 'cb'), may hold values from -0.125 to 0.125
- down_second: bfloat16 [11264, 4096], P('cb', 'ra'), may hold values from -0.078125 to 0.078125
- post_gain_second: float32 [4096], P('ra'), may hold values from 0.1 to 1.9
Outputs:
- mixed: bfloat16 [512, 4096], P(None, 'ra')
The draws below stay inside these ranges and needn't reach their ends.
Inputs may be any that keep to these rules, and one draw needn't show every extreme that they name: `tokens`: each block of 128 consecutive channels has its own scale, and rows have their own scales.
All inputs are finite; a program needn't handle non-finite values.
Results may differ from the reference program's by a relative error of at most 0.0071.
Values may be sent and summed in bfloat16 or wider, within the bound.
No kernel may reach another device: no remote copies, remote signals or barrier semaphores. Data moves between devices by JAX's collectives and lax.ppermute only.
A program may use at most 64 MiB of HBM per device.

```python
import jax
import jax.numpy as jnp
from jax import lax

D = 4096
FF = 11264
TOKENS = 512


def draw_tokens(key, part):
    base_key = jax.random.fold_in(key, 11)
    key_noise, key_block, key_row, key_common = jax.random.split(base_key, 4)
    noise = jax.random.normal(key_noise, (TOKENS, D), jnp.float32)
    block_scale = jnp.exp(jax.random.uniform(key_block, (32,), jnp.float32, jnp.log(0.15), jnp.log(0.6)))
    column_scale = jnp.repeat(block_scale, D // 32)
    row_scale = jax.random.uniform(key_row, (TOKENS, 1), jnp.float32, 0.7, 1.4)
    values = noise * column_scale[None, :] * row_scale
    return jnp.clip(values, -4.0, 4.0).astype(jnp.bfloat16)


def spiked(drawn, key, source, target, parts, factor):
    owner, partner = [(jnp.arange(drawn.shape[dim]) // (drawn.shape[dim] // parts)).reshape([-1 if axis == dim else 1 for axis in range(drawn.ndim)]) for dim in (source, target)]
    chosen = jax.random.permutation(key, parts)[partner]
    strong = (owner == chosen) | (owner == (partner + parts // 2) % parts)
    return jnp.where(strong, factor * drawn, drawn)


def level_of(own_key, shape, cuts, low, top_value):
    factor_of = 1.0
    for position, blocks in cuts:
        heights = jax.random.uniform(jax.random.fold_in(jax.random.fold_in(own_key, 6), position), (blocks,), jnp.float32, low / len(cuts), top_value / len(cuts))
        factor_of = factor_of * jnp.repeat(jnp.exp(heights), shape[position] // blocks).reshape((-1,) + (1,) * (len(shape) - 1 - position))
    return factor_of


def gaussian_with(key, dims, spread, bound, cuts, heavy, kind=jnp.bfloat16):
    result = spread * jax.random.normal(key, dims, jnp.float32)
    if cuts:
        result = result * level_of(key, dims, cuts, -0.22, 0.18)
    return jnp.clip(spiked(result, jax.random.fold_in(key, 3), *heavy), -bound, bound).astype(kind)


def setup_inputs(seed: int = 0) -> dict:
    arg_keys = jax.random.split(jax.random.key(seed), 12)
    tokens = draw_tokens(jax.random.fold_in(arg_keys[11], 71), 0)
    pre_gain_first = jnp.clip(1.0 + 0.18 * jax.random.normal(arg_keys[1], (D,), jnp.float32), 0.1, 1.9)
    gate_first = gaussian_with(arg_keys[2], (D, FF), D ** -0.5, 0.125, ((0, 8), (1, 4)), (0, 1, 8, 2.0))
    up_first = gaussian_with(arg_keys[3], (D, FF), D ** -0.5, 0.125, ((0, 8), (1, 4)), (0, 1, 8, 2.0))
    down_first = gaussian_with(arg_keys[4], (FF, D), FF ** -0.5, 0.078125, ((0, 4), (1, 8)), (0, 1, 8, 2.0))
    post_gain_first = jnp.clip(1.0 + 0.18 * jax.random.normal(arg_keys[5], (D,), jnp.float32), 0.1, 1.9)
    pre_gain_second = jnp.clip(1.0 + 0.18 * jax.random.normal(arg_keys[6], (D,), jnp.float32), 0.1, 1.9)
    gate_second = gaussian_with(arg_keys[7], (D, FF), D ** -0.5, 0.125, ((0, 8), (1, 4)), (0, 1, 8, 2.0))
    up_second = gaussian_with(arg_keys[8], (D, FF), D ** -0.5, 0.125, ((0, 8), (1, 4)), (0, 1, 8, 2.0))
    down_second = gaussian_with(arg_keys[9], (FF, D), FF ** -0.5, 0.078125, ((0, 4), (1, 8)), (0, 1, 8, 2.0))
    post_gain_second = jnp.clip(1.0 + 0.18 * jax.random.normal(arg_keys[10], (D,), jnp.float32), 0.1, 1.9)
    return dict(tokens=tokens, pre_gain_first=pre_gain_first, gate_first=gate_first, up_first=up_first, down_first=down_first, post_gain_first=post_gain_first, pre_gain_second=pre_gain_second, gate_second=gate_second, up_second=up_second, down_second=down_second, post_gain_second=post_gain_second)


EPS = 1e-06

def row_scale(values):
    return lax.rsqrt(lax.optimization_barrier(jnp.mean(values * values, axis=-1, keepdims=True)) + EPS)

def half_step(resid, pre_gain, gate_weight, up_weight, down_weight, post_gain):
    normed = (resid * row_scale(resid) * pre_gain).astype(jnp.bfloat16)
    gate_value = jnp.dot(normed, gate_weight, preferred_element_type=jnp.float32)
    up_value = jnp.dot(normed, up_weight, preferred_element_type=jnp.float32)
    hidden = (jax.nn.silu(gate_value) * up_value).astype(jnp.bfloat16)
    branch = jnp.dot(hidden, down_weight, preferred_element_type=jnp.float32)
    return resid + 0.5 * branch * row_scale(branch) * post_gain

def reference(tokens, pre_gain_first, gate_first, up_first, down_first, post_gain_first, pre_gain_second, gate_second, up_second, down_second, post_gain_second):
    resid = tokens.astype(jnp.float32)
    middle = half_step(resid, pre_gain_first, gate_first, up_first, down_first, post_gain_first)
    final = half_step(middle, pre_gain_second, gate_second, up_second, down_second, post_gain_second)
    return final.astype(jnp.bfloat16)
```

```python
import jax
import jax.numpy as jnp
from jax import lax
from jax.sharding import PartitionSpec as P

EPS = 1e-06
LANES = 128
CHUNKS = 4


def flip(value, axis, distance):
    size = lax.axis_size(axis)
    return lax.ppermute(value, axis, [(i, i ^ distance) for i in range(size)])


def all_sum(value, axis):
    size = lax.axis_size(axis)
    step = 1
    while step < size:
        radix = min(8, size // step)
        parts = [flip(value, axis, k * step) for k in range(1, radix)]
        for part in parts:
            value = value + part
        step *= radix
    return value


def mirror(position, size):
    result, step = 0, 1
    while step < size:
        result = result * 2 + (position // step) % 2
        step *= 2
    return result


def to_relative(value):
    size = lax.axis_size("ra")
    rows = value.shape[0] // size
    own = lax.axis_index("ra")
    return jnp.concatenate(
        [
            lax.dynamic_slice_in_dim(value, (own ^ mirror(p, size)) * rows, rows, 0)
            for p in range(size)
        ],
        axis=0,
    )


def to_absolute(value):
    size = lax.axis_size("ra")
    rows = value.shape[0] // size
    own = lax.axis_index("ra")
    pieces = []
    for block in range(size):
        other = own ^ block
        position, step = jnp.zeros_like(own), 1
        while step < size:
            position = position * 2 + (other // step) % 2
            step *= 2
        pieces.append(lax.dynamic_slice_in_dim(value, position * rows, rows, 0))
    return jnp.concatenate(pieces, axis=0)


def scatter_sum(value):
    size = lax.axis_size("ra")
    distance = 1
    while distance < size:
        half = value.shape[0] // 2
        came = flip(value[half:].astype(jnp.bfloat16), "ra", distance)
        value = value[:half] + came.astype(jnp.float32)
        distance *= 2
    return value


def gather_rows(value):
    distance = lax.axis_size("ra") // 2
    while distance >= 1:
        value = jnp.concatenate([value, flip(value, "ra", distance)], axis=0)
        distance //= 2
    return value


def cuts_of(width):
    units = width // LANES
    count = min(CHUNKS, units)
    edges = [(units * k // count) * LANES for k in range(count)]
    return list(zip(edges, edges[1:] + [width]))


def branch_slab(normed, scale, gate_weight, up_weight, down_weight):
    relative = to_relative(normed)
    partial_out = None
    for low, high in cuts_of(gate_weight.shape[1]):
        gate_value = jnp.dot(relative, gate_weight[:, low:high], preferred_element_type=jnp.float32)
        up_value = jnp.dot(relative, up_weight[:, low:high], preferred_element_type=jnp.float32)
        both = scatter_sum(jnp.concatenate([gate_value, up_value], axis=1)) * scale
        gate_sum, up_sum = both[:, : high - low], both[:, high - low :]
        hidden = gather_rows((jax.nn.silu(gate_sum) * up_sum).astype(jnp.bfloat16))
        part = jnp.dot(hidden, down_weight[low:high], preferred_element_type=jnp.float32)
        partial_out = part if partial_out is None else partial_out + part
    out = to_absolute(partial_out.astype(jnp.bfloat16))
    groups = lax.axis_size("cb")
    rows, cols = out.shape
    parts = lax.all_to_all(out, "cb", 0, 0, tiled=True).reshape(groups, rows // groups, cols)
    return jnp.sum(parts.astype(jnp.float32), axis=0)


def row_squares(value):
    return jnp.sum(value * value, axis=1)


def body(
    tokens,
    pre_gain_first,
    gate_first,
    up_first,
    down_first,
    post_gain_first,
    pre_gain_second,
    gate_second,
    up_second,
    down_second,
    post_gain_second,
):
    count = tokens.shape[0]
    width = tokens.shape[1] * lax.axis_size("ra")
    slab = count // lax.axis_size("cb")
    block = count // lax.axis_size("ra")
    slab_start = lax.axis_index("cb") * slab
    block_start = lax.axis_index("ra") * block

    def row_scale(total):
        return lax.rsqrt(total / width + EPS)

    def own_block_scale(total):
        return row_scale(lax.dynamic_slice_in_dim(total, block_start, block, 0))[:, None]

    def half_step(resid, branch, post_gain):
        total = all_sum(row_squares(branch), "ra")
        return resid + 0.5 * row_scale(total)[:, None] * branch * post_gain[None, :]

    full = tokens.astype(jnp.float32)
    first_in = (full * pre_gain_first[None, :]).astype(jnp.bfloat16)
    first_scale = own_block_scale(all_sum(row_squares(full), "ra"))
    branch = branch_slab(first_in, first_scale, gate_first, up_first, down_first)

    resid = lax.dynamic_slice_in_dim(tokens, slab_start, slab, 0).astype(jnp.float32)
    middle = half_step(resid, branch, post_gain_first)
    second_slab = (middle * pre_gain_second[None, :]).astype(jnp.bfloat16)
    second_in = lax.all_gather(second_slab, "cb", axis=0, tiled=True)
    placed = lax.dynamic_update_slice_in_dim(
        jnp.zeros((count,), jnp.float32), row_squares(middle), slab_start, 0
    )
    second_scale = own_block_scale(all_sum(all_sum(placed, "ra"), "cb"))
    branch = branch_slab(second_in, second_scale, gate_second, up_second, down_second)
    mixed = half_step(middle, branch, post_gain_second).astype(jnp.bfloat16)
    return lax.all_gather(mixed, "cb", axis=0, tiled=True)


def solution(mesh):
    in_specs = (
        P(None, "ra"),
        P("ra"),
        P("ra", "cb"),
        P("ra", "cb"),
        P("cb", "ra"),
        P("ra"),
        P("ra"),
        P("ra", "cb"),
        P("ra", "cb"),
        P("cb", "ra"),
        P("ra"),
    )
    out_specs = P(None, "ra")
    return jax.shard_map(body, mesh=mesh, in_specs=in_specs, out_specs=out_specs, check_vma=False)
```

```python
import jax
import jax.numpy as jnp
from jax import lax
from jax.sharding import PartitionSpec as P

EPS = 1e-06
LANES = 128
CHUNKS = 4


def flip(value, axis, distance):
    size = lax.axis_size(axis)
    return lax.ppermute(value, axis, [(i, i ^ distance) for i in range(size)])


def all_sum(value, axis):
    size = lax.axis_size(axis)
    step = 1
    while step < size:
        radix = min(8, size // step)
        parts = [flip(value, axis, k * step) for k in range(1, radix)]
        for part in parts:
            value = value + part
        step *= radix
    return value


def mirror(position, size):
    result, step = 0, 1
    while step < size:
        result = result * 2 + (position // step) % 2
        step *= 2
    return result


def to_relative(value):
    size = lax.axis_size("ra")
    rows = value.shape[0] // size
    own = lax.axis_index("ra")
    return jnp.concatenate(
        [
            lax.dynamic_slice_in_dim(value, (own ^ mirror(p, size)) * rows, rows, 0)
            for p in range(size)
        ],
        axis=0,
    )


def to_absolute(value):
    size = lax.axis_size("ra")
    rows = value.shape[0] // size
    own = lax.axis_index("ra")
    pieces = []
    for block in range(size):
        other = own ^ block
        position, step = jnp.zeros_like(own), 1
        while step < size:
            position = position * 2 + (other // step) % 2
            step *= 2
        pieces.append(lax.dynamic_slice_in_dim(value, position * rows, rows, 0))
    return jnp.concatenate(pieces, axis=0)


def scatter_rest(value, came):
    size = lax.axis_size("ra")
    value = value + came.astype(jnp.float32)
    distance = 2
    while distance < size:
        half = value.shape[0] // 2
        came = flip(value[half:].astype(jnp.bfloat16), "ra", distance)
        value = value[:half] + came.astype(jnp.float32)
        distance *= 2
    return value


def gather_rows(value):
    distance = lax.axis_size("ra") // 2
    while distance >= 1:
        value = jnp.concatenate([value, flip(value, "ra", distance)], axis=0)
        distance //= 2
    return value


def cuts_of(width):
    units = width // LANES
    count = min(CHUNKS, units)
    edges = [(units * k // count) * LANES for k in range(count)]
    return list(zip(edges, edges[1:] + [width]))


def branch_slab(normed, gate_weight, up_weight, down_weight):
    relative = to_relative(normed)
    half = relative.shape[0] // 2
    cuts = cuts_of(gate_weight.shape[1])
    kept, received = [], []
    for low, high in cuts:
        gate_value = jnp.dot(relative, gate_weight[:, low:high], preferred_element_type=jnp.float32)
        up_value = jnp.dot(relative, up_weight[:, low:high], preferred_element_type=jnp.float32)
        both = jnp.concatenate([gate_value, up_value], axis=1)
        sent = both[half:].astype(jnp.bfloat16)
        relative, sent = lax.optimization_barrier((relative, sent))
        kept.append(both[:half])
        received.append(flip(sent, "ra", 1))
    partial_out = None
    for k, (low, high) in enumerate(cuts):
        came = received[k]
        if k:
            came, _ = lax.optimization_barrier((came, received[k - 1]))
        both = scatter_rest(kept[k], came)
        gate_sum, up_sum = both[:, : high - low], both[:, high - low :]
        hidden = gather_rows((jax.nn.silu(gate_sum) * up_sum).astype(jnp.bfloat16))
        part = jnp.dot(hidden, down_weight[low:high], preferred_element_type=jnp.float32)
        partial_out = part if partial_out is None else partial_out + part
    out = to_absolute(partial_out.astype(jnp.bfloat16))
    groups = lax.axis_size("cb")
    rows, cols = out.shape
    parts = lax.all_to_all(out, "cb", 0, 0, tiled=True).reshape(groups, rows // groups, cols)
    return jnp.sum(parts.astype(jnp.float32), axis=0)


def row_squares(value):
    return jnp.sum(value * value, axis=1)


def body(
    tokens,
    pre_gain_first,
    gate_first,
    up_first,
    down_first,
    post_gain_first,
    pre_gain_second,
    gate_second,
    up_second,
    down_second,
    post_gain_second,
):
    count = tokens.shape[0]
    width = tokens.shape[1] * lax.axis_size("ra")
    slab = count // lax.axis_size("cb")
    slab_start = lax.axis_index("cb") * slab

    def row_scale(total):
        return lax.rsqrt(total / width + EPS)

    def normed(value, gain):
        scale = row_scale(all_sum(row_squares(value), "ra"))
        return (value * scale[:, None] * gain[None, :]).astype(jnp.bfloat16)

    def half_step(resid, branch, post_gain):
        total = all_sum(row_squares(branch), "ra")
        return resid + 0.5 * row_scale(total)[:, None] * branch * post_gain[None, :]

    full = tokens.astype(jnp.float32)
    first_in = normed(full, pre_gain_first)
    branch = branch_slab(first_in, gate_first, up_first, down_first)

    resid = lax.dynamic_slice_in_dim(tokens, slab_start, slab, 0).astype(jnp.float32)
    middle = half_step(resid, branch, post_gain_first)
    second_in = lax.all_gather(normed(middle, pre_gain_second), "cb", axis=0, tiled=True)
    branch = branch_slab(second_in, gate_second, up_second, down_second)
    mixed = half_step(middle, branch, post_gain_second).astype(jnp.bfloat16)
    return lax.all_gather(mixed, "cb", axis=0, tiled=True)


def solution(mesh):
    in_specs = (
        P(None, "ra"),
        P("ra"),
        P("ra", "cb"),
        P("ra", "cb"),
        P("cb", "ra"),
        P("ra"),
        P("ra"),
        P("ra", "cb"),
        P("ra", "cb"),
        P("cb", "ra"),
        P("ra"),
    )
    out_specs = P(None, "ra")
    return jax.shard_map(body, mesh=mesh, in_specs=in_specs, out_specs=out_specs, check_vma=False)
```
